32 devices in a mesh: gr: 2 (over y), fs: 4 (over z), tp: 4 (over x, core).
Axes of the slice: x: 2, y: 2, z: 4, core: 2. Of those that a mesh axis runs over, the one named last changes fastest.
Arguments:
- prompt: bfloat16 [4096, 2048], P(('gr', 'fs')), may hold values from -6 to 6
- norm_gain: float32 [2048], P(('gr', 'fs')), may hold values from 0.1 to 1.9
- gate_master: float32 [32, 2048, 1024], P(None, ('gr', 'fs'), 'tp'), may hold values from -6 to 6
- up_master: float32 [32, 2048, 1024], P(None, ('gr', 'fs'), 'tp'), may hold values from -6 to 6
- down_master: float32 [32, 2048, 1024], P(None, ('gr', 'fs'), 'tp'), may hold values from -6 to 6
- routes: int32 [4096, 2], P(('gr', 'fs')), may hold values from 0 to 31, as said below
- route_weights: float32 [4096, 2], P(('gr', 'fs')), may hold values from 0.1 to 0.9
Outputs:
- gate_ready: bfloat16 [32, 2048, 1024], P('fs', None, 'tp')
- up_ready: bfloat16 [32, 2048, 1024], P('fs', None, 'tp')
- down_ready: bfloat16 [32, 2048, 1024], P('fs', None, 'tp')
- blended: bfloat16 [4096, 2048], P(('gr', 'fs'), 'tp')
The draws below stay inside these ranges and needn't reach their ends.
Inputs may be any that keep to these rules, and one draw needn't show every extreme that they name: `routes`: each row names 2 different experts of one group: expert // 8 is the group. In every aligned block of 512 rows (the tokens of one index of gr and fs) half of the rows choose one group, and no expert is named more than 64 times; in every block some expert is named exactly 64 times.
All inputs are finite; a program needn't handle non-finite values.
Results may differ from the reference program's by a relative error of at most 0.015.
Values may be sent and summed in bfloat16 or wider, within the bound.
A program may use at most 128 MiB of HBM per device.

```python
import jax
import jax.numpy as jnp
from jax import lax

D = 2048
FF = 1024
N_GROUPS = 4
PER_GROUP = 8
TOP = 2
N_EXPERTS = 32
TOK_DEV = 512
CAP = 64
TOKENS = 4096
N_TP = 4


def draw_routes(key, part):
    blocks = TOKENS // TOK_DEV
    half_block = TOK_DEV // 2
    subkeys = jax.random.split(jax.random.fold_in(key, 7), 8)
    common = jax.random.randint(subkeys[0], (), 0, N_GROUPS)
    own_big = jax.random.randint(subkeys[1], (blocks,), 0, N_GROUPS)
    big_group = jnp.where(jnp.arange(blocks) < blocks // 2, common, own_big)
    cut_points = jnp.sort(jax.random.randint(subkeys[2], (blocks, N_GROUPS - 2), 0, half_block + 1), axis=1)
    edges = jnp.concatenate([jnp.zeros((blocks, 1), jnp.int32), cut_points.astype(jnp.int32), jnp.full((blocks, 1), half_block, jnp.int32)], axis=1)
    small_sizes = edges[:, 1:] - edges[:, :-1]
    groups = jnp.arange(N_GROUPS, dtype=jnp.int32)
    offset = (groups[None, :] - big_group[:, None] - 1) % N_GROUPS
    group_sizes = jnp.where(offset == N_GROUPS - 1, half_block, jnp.take_along_axis(small_sizes, jnp.minimum(offset, N_GROUPS - 2), axis=1))
    group_ends = jnp.cumsum(group_sizes, axis=1)
    starts = group_ends - group_sizes
    token_ranks = jnp.argsort(jax.random.randint(subkeys[3], (blocks, TOK_DEV), 0, 1 << 20) * TOK_DEV + jnp.arange(TOK_DEV, dtype=jnp.int32)[None, :], axis=1)
    group_of = jnp.sum((token_ranks[:, :, None] >= group_ends[:, None, :]).astype(jnp.int32), axis=2)
    inner_rank = token_ranks - jnp.take_along_axis(starts, group_of, axis=1)
    first_shift = jax.random.randint(subkeys[4], (blocks, N_GROUPS), 0, PER_GROUP)
    second_step = jax.random.randint(subkeys[5], (blocks, N_GROUPS), 1, PER_GROUP)
    local_order = jnp.argsort(jax.random.randint(subkeys[6], (blocks, N_GROUPS, PER_GROUP), 0, 1 << 20) * PER_GROUP + jnp.arange(PER_GROUP, dtype=jnp.int32), axis=2)
    first_local = (inner_rank + jnp.take_along_axis(first_shift, group_of, axis=1)) % PER_GROUP
    second_local = (first_local + jnp.take_along_axis(second_step, group_of, axis=1)) % PER_GROUP
    group_table = local_order[jnp.arange(blocks)[:, None], group_of]
    local_pair = jnp.take_along_axis(group_table, jnp.stack([first_local, second_local], axis=2), axis=2)
    experts = group_of[:, :, None] * PER_GROUP + local_pair
    return experts.reshape(TOKENS, TOP).astype(jnp.int32)


def steps_of(own_key, extent, shards, least, largest):
    def one(dim, shards_of):
        heights = jax.random.uniform(jax.random.fold_in(jax.random.fold_in(own_key, 6), dim), (shards_of,), jnp.float32, least / len(shards), largest / len(shards))
        return jnp.repeat(jnp.exp(heights), extent[dim] // shards_of).reshape((-1,) + (1,) * (len(extent) - dim - 1))

    loudness = one(*shards[0])
    for cut in shards[1:]:
        loudness = loudness * one(*cut)
    return loudness


def gaussian(key, dims, width, reach, cuts=(), held_as=jnp.bfloat16):
    entries = jax.random.normal(key, dims, jnp.float32) * width
    if len(cuts) > 0:
        entries = steps_of(key, dims, cuts, -0.22, 0.18) * entries
    return jnp.clip(entries, min=-reach, max=reach).astype(held_as)


def setup_inputs(seed: int = 0) -> dict:
    streams_of = jax.random.split(jax.random.key(seed), 8)
    return {
        "prompt": gaussian(streams_of[0], (TOKENS, D), 1.0, 6.0, ((0, 8),)),
        "norm_gain": jnp.clip(1.0 + 0.18 * jax.random.normal(streams_of[1], (D,), jnp.float32), 0.1, 1.9),
        "gate_master": gaussian(streams_of[2], (N_EXPERTS, D, FF), 1.0, 6.0, ((1, 8), (2, 4)), jnp.float32),
        "up_master": gaussian(streams_of[3], (N_EXPERTS, D, FF), 1.0, 6.0, ((1, 8), (2, 4)), jnp.float32),
        "down_master": gaussian(streams_of[4], (N_EXPERTS, D, FF), 1.0, 6.0, ((1, 8), (2, 4)), jnp.float32),
        "routes": draw_routes(jax.random.fold_in(streams_of[7], 71), 0),
        "route_weights": jnp.clip(0.1 + 0.79999997 * jax.random.uniform(streams_of[6], (TOKENS, TOP), jnp.float32) ** steps_of(streams_of[6], (TOKENS, TOP), ((0, 8),), -0.2, 0.2), 0.1, 0.9),
    }


EPS = 1e-06

def reference(prompt, norm_gain, gate_master, up_master, down_master, routes, route_weights):
    gate_new = (norm_gain[None, :, None] * gate_master).astype(jnp.bfloat16)
    up_new = (norm_gain[None, :, None] * up_master).astype(jnp.bfloat16)
    down_new = down_master.astype(jnp.bfloat16)
    prompt_wide = prompt.astype(jnp.float32)
    normed = (prompt_wide * lax.rsqrt(lax.optimization_barrier(jnp.mean(prompt_wide * prompt_wide, axis=-1, keepdims=True)) + EPS)).astype(jnp.bfloat16)
    route_list = routes.reshape(-1).astype(jnp.int32)
    route_hits = (route_list[:, None] == jnp.arange(N_EXPERTS, dtype=jnp.int32)[None, :]).astype(jnp.int32)
    slot_rank = lax.optimization_barrier(jnp.sum((jnp.cumsum(route_hits, axis=0).astype(jnp.int32) - 1) * route_hits, axis=1)).astype(jnp.int32)
    expert_room = TOKENS // TOK_DEV * CAP
    slot_index = (route_list * expert_room + slot_rank).astype(jnp.int32)
    token_of = (jnp.arange(route_list.shape[0], dtype=jnp.int32) // TOP).astype(jnp.int32)
    slot_owner = jnp.zeros((N_EXPERTS * expert_room,), jnp.int32).at[slot_index].set(token_of)

    def expert(operands):
        row_ids, gate_rows, up_rows, down_rows = operands
        picked = normed[row_ids]
        pre_gate = jnp.dot(picked, gate_rows, preferred_element_type=jnp.float32) * D ** (-0.5)
        pre_up = jnp.dot(picked, up_rows, preferred_element_type=jnp.float32) * D ** (-0.5)
        hidden = (jax.nn.silu(pre_gate) * pre_up).astype(jnp.bfloat16)
        hidden_blocks = hidden.astype(jnp.float32).reshape(row_ids.shape[0], N_TP, FF // N_TP)
        down_blocks = down_rows.astype(jnp.float32).reshape(D, N_TP, FF // N_TP)
        partial_value = (jnp.einsum('rnf,dnf->rnd', hidden_blocks, down_blocks) * FF ** (-0.5)).astype(jnp.bfloat16)
        return lax.optimization_barrier(jnp.sum(partial_value.astype(jnp.float32), axis=1)).astype(jnp.bfloat16)
    results = lax.map(expert, (slot_owner.reshape(N_EXPERTS, expert_room), gate_new, up_new, down_new))
    per_choice = results.reshape(N_EXPERTS * expert_room, D)[slot_index].reshape(TOKENS, TOP, D)
    blended = lax.optimization_barrier(jnp.sum(per_choice.astype(jnp.float32) * route_weights[:, :, None], axis=1))
    return (gate_new, up_new, down_new, blended.astype(jnp.bfloat16))
```

```python
import functools

import jax
import jax.numpy as jnp
from jax import lax
from jax.experimental import pallas as pl
from jax.experimental.pallas import tpu as pltpu
from jax.sharding import PartitionSpec as P

EPS = 1e-06
GROUP = 8
MESH = pl.DeviceIdType.MESH
SLOTS = 4
PIECES = 6
EARLY = 2


def kernel(
    dims, gain, routes, rw, prompt, gm, um, dm, g_out, u_out, d_out, ans, slot_out,
    stage, wb, x, w, pr_in, nq, tok, wsend, gb, hid, yr, ys,
    st_sem, zs, zr, vs, vr, tzs, tzr, wzs, wzr, txs, txr, tw_sem, ps, pr, rs, rr,
):
    gr, fs, tp, experts, rows, width, cap, depth, hidden_all, split = dims
    me_g, me_f, me_t = lax.axis_index("gr"), lax.axis_index("fs"), lax.axis_index("tp")
    bf16, f32 = jnp.bfloat16, jnp.float32
    local = experts // fs
    half = local // 2
    groups = experts // GROUP
    quarter = depth // tp
    total = fs * cap
    tokens = prompt.shape[0]
    tile = min(256, cap)
    sub = rows // split
    apart = sub % 128 == 0
    masters, outs = (gm, um, dm), (g_out, u_out, d_out)

    def fs_at(k):
        return lax.rem(me_f + k, fs)

    def fs_from(k):
        return lax.rem(me_f + fs - k, fs)

    def gr_at(j):
        return lax.rem(me_g + j, gr)

    def remote(src, dst, ssem, rsem, where):
        return pltpu.make_async_remote_copy(
            src_ref=src, dst_ref=dst, send_sem=ssem, recv_sem=rsem,
            device_id=where, device_id_type=MESH,
        )

    def matrix(s):
        return (0, 1, 0, 1, 2, 2)[s]

    def half_of(s):
        return (0, 0, 1, 1, 0, 1)[s]

    def parts(s):
        h = half_of(s)
        if s >= 4 and split > 1:
            n = max(1, local // 4)
            return [(q * n, n, q * n, h * sub, sub) for q in range(local // n)]
        return [(q * half, half, h * half, q * sub, sub) for q in range(split)]

    def region(s, g, f, q):
        _, n, e0, r0, nr = parts(s)[q]
        at = pl.multiple_of((g * fs + f) * rows + r0, nr)
        return outs[matrix(s)].at[pl.ds(e0, n), pl.ds(at, nr), :]

    def buffered(s, k, q):
        b0, n, _, _, _ = parts(s)[q]
        return wb.at[s, k - 1, pl.ds(b0, n)]

    barrier = pltpu.get_barrier_semaphore()
    for k in range(1, fs):
        pl.semaphore_signal(barrier, inc=1, device_id={"fs": fs_at(k)}, device_id_type=MESH)
    for j in range(1, gr):
        pl.semaphore_signal(barrier, inc=1, device_id={"gr": gr_at(j)}, device_id_type=MESH)
    for j in range(1, tp):
        pl.semaphore_signal(
            barrier, inc=1, device_id={"tp": lax.rem(me_t + j, tp)}, device_id_type=MESH
        )

    if fs == 4:
        odd, side = lax.rem(me_f, 2), lax.rem(me_t, 2)
        near, far = 1 + 2 * odd, 3 - 2 * odd
        sending = [
            jnp.where(side == 0, 2, near), jnp.where(side == 0, far, 2), jnp.where(side == 0, near, far)
        ]
        hearing = [2, 1, 3]
    else:
        sending = list(range(1, fs))
        hearing = sending
    items = [(s, k) for s in range(PIECES) for k in [0] + sending]

    def load(i):
        s, k = items[i]
        first = fs_at(k) * local
        slot = i % SLOTS
        if s >= 4 and split > 1:
            cuts = [(0, local, 0, half_of(s) * sub)]
        else:
            cuts = [(q * half, half, half_of(s) * half, q * sub) for q in range(split)]
        return [
            pltpu.make_async_copy(
                masters[matrix(s)].at[pl.ds(first + e0, n), pl.ds(r0, sub)],
                stage.at[slot, pl.ds(b0, n)], st_sem.at[slot, c],
            )
            for c, (b0, n, e0, r0) in enumerate(cuts)
        ]

    for i in range(SLOTS):
        for c in load(i):
            c.start()
    prompt_copy = pltpu.make_async_copy(prompt, pr_in, tw_sem.at[0])
    prompt_copy.start()
    square = (rows, rows)
    diagonal = lax.broadcasted_iota(jnp.int32, square, 0) == lax.broadcasted_iota(jnp.int32, square, 1)
    column = jnp.sum(jnp.where(diagonal, gain[...], 0.0), axis=1, keepdims=True)
    gb[...] = jnp.broadcast_to(column, gb.shape)
    pl.semaphore_wait(barrier, (fs - 1) + (gr - 1) + (tp - 1))

    def z_copy(s, k, q):
        return remote(
            buffered(s, k, q), region(s, me_g, me_f, q), zs.at[s, k, q], zr.at[s, k, q],
            {"fs": fs_at(k)},
        )

    def z_landed(s, k, q):
        f = fs_from(k)
        ref = region(s, me_g, f, q)
        return remote(ref, ref, zs.at[s, k, q], zr.at[s, k, q], {"fs": f})

    def v_copy(s, k, j, q):
        ref = region(s, me_g, fs_from(k), q)
        return remote(ref, ref, vs.at[s, k, j - 1, q], vr.at[s, k, j - 1, q], {"gr": gr_at(j)})

    def v_landed(s, k, j, q):
        g = lax.rem(me_g + gr - j, gr)
        ref = region(s, g, fs_from(k), q)
        return remote(ref, ref, vs.at[s, k, j - 1, q], vr.at[s, k, j - 1, q], {"gr": g})

    def send_gr(s, k):
        for q in range(len(parts(s))):
            for j in range(1, gr):
                v_copy(s, k, j, q).start()

    def forward(s, k):
        for q in range(len(parts(s))):
            z_landed(s, k, q).wait_recv()
            for j in range(1, gr):
                v_copy(s, k, j, q).start()

    def arrived_gr(s, k):
        for q in range(len(parts(s))):
            for j in range(1, gr):
                v_landed(s, k, j, q).wait_recv()

    def cast_item(i):
        s, k = items[i]
        m, h, slot = matrix(s), half_of(s), i % SLOTS
        own = isinstance(k, int) and k == 0
        for c in load(i):
            c.wait()
        base = (me_g * fs + me_f) * rows
        if s >= 4 and split > 1:
            cuts = [(0, local, 0, h * sub)]
        else:
            cuts = [(q * half, half, h * half, q * sub) for q in range(split)]
        for b0, n, e0, r0 in cuts:
            scale = None
            if m < 2:
                scale = jnp.concatenate([gb[pl.ds(r0, sub)]] * (width // 128), axis=1)

            def cast(e, carry, b0=b0, e0=e0, r0=r0, scale=scale):
                value = stage[slot, b0 + e]
                if scale is not None:
                    value = scale * value
                if own:
                    at = pl.multiple_of(base + r0, sub)
                    outs[m][e0 + e, pl.ds(at, sub), :] = value.astype(bf16)
                else:
                    wb[s, k - 1, b0 + e] = value.astype(bf16)
                return carry

            lax.fori_loop(0, n, cast, 0)
        if i + SLOTS < len(items):
            for c in load(i + SLOTS):
                c.start()
        if own:
            if s < 3:
                send_gr(s, 0)
        else:
            for q in range(len(parts(s))):
                z_copy(s, k, q).start()

    def x_block(f, t):
        return x.at[
            pl.ds(pl.multiple_of(f * cap, cap), cap),
            pl.ds(pl.multiple_of(t * quarter, quarter), quarter),
        ]

    def w_block(f):
        return w.at[:, pl.ds(pl.multiple_of(f * cap, cap), cap)]

    def tok_copy(k):
        dst = fs_at(k)
        return remote(tok.at[(dst * local) // GROUP], x_block(me_f, me_t), tzs.at[k], tzr.at[k], {"fs": dst})

    def w_copy(k):
        dst = fs_at(k)
        return remote(wsend.at[dst], w_block(me_f), wzs.at[k], wzr.at[k], {"fs": dst})

    def tx_copy(k, j):
        ref = x_block(fs_from(k), me_t)
        return remote(ref, ref, txs.at[k, j], txr.at[k, j], {"tp": lax.rem(me_t + j, tp)})

    def prepare():
        prompt_copy.wait()
        step = min(64, tokens)
        mine = pl.ds(pl.multiple_of(me_t * quarter, quarter), quarter)

        def norm(r, carry):
            at = pl.ds(pl.multiple_of(r * step, step), step)
            wide = pr_in[at, :].astype(f32)
            scale = lax.rsqrt(jnp.mean(wide * wide, axis=-1, keepdims=True) + EPS)
            nq[at, :] = (pr_in[at, mine].astype(f32) * scale).astype(bf16)
            return carry

        lax.fori_loop(0, tokens // step, norm, 0)
        first, second = routes[0:1, :], routes[1:2, :]
        pad = max(8, groups)
        low = GROUP * lax.broadcasted_iota(jnp.int32, (pad, tokens), 0)
        hits = jnp.logical_and(first >= low, first < low + GROUP)
        flat = (tokens, tokens)
        before = lax.broadcasted_iota(jnp.int32, flat, 0) < lax.broadcasted_iota(jnp.int32, flat, 1)
        counts = jnp.dot(
            jnp.where(hits, 1.0, 0.0).astype(bf16), jnp.where(before, 1.0, 0.0).astype(bf16),
            preferred_element_type=f32,
        )
        lead = (lax.broadcasted_iota(jnp.int32, (pad, tokens), 0) * cap).astype(f32)
        slot = jnp.sum(jnp.where(hits, counts + lead, 0.0), axis=0, keepdims=True).astype(jnp.int32)
        slot_out[...] = slot
        for g in range(groups):
            spots = lax.broadcasted_iota(jnp.int32, (cap, tokens), 0) + g * cap
            place = jnp.where(spots == slot, 1.0, 0.0).astype(bf16)
            packed = jnp.dot(place, nq[...], preferred_element_type=f32).astype(bf16)
            tok[g] = packed

            @pl.when((me_f * local) // GROUP == g)
            def _(packed=packed):
                x[pl.ds(pl.multiple_of(me_f * cap, cap), cap), mine] = packed

            for d in range(fs):
                if (d * local) // GROUP != g:
                    continue
                named = lax.broadcasted_iota(jnp.int32, (w.shape[0], tokens), 0) + d * local
                spread = jnp.where(first == named, rw[0:1, :], 0.0)
                spread += jnp.where(second == named, rw[1:2, :], 0.0)
                packed_w = jnp.zeros((w.shape[0], cap), f32)
                for _ in range(3):
                    top = spread.astype(bf16)
                    packed_w += lax.dot_general(
                        top, place, (((1,), (1,)), ((), ())), preferred_element_type=f32
                    )
                    spread = spread - top.astype(f32)
                wsend[d] = packed_w

                @pl.when(me_f == d)
                def _(packed_w=packed_w):
                    w[:, pl.ds(pl.multiple_of(me_f * cap, cap), cap)] = packed_w

        for k in range(1, fs):
            tok_copy(k).start()
            w_copy(k).start()
        for j in range(1, tp):
            tx_copy(0, j).start()

    per = len(items) // PIECES
    for i in range(EARLY * per):
        cast_item(i)
    prepare()
    for i in range(EARLY * per, len(items)):
        cast_item(i)

    def tokens_on(k):
        f = fs_from(k)
        remote(x_block(f, me_t), x_block(f, me_t), tzs.at[k], tzr.at[k], {"fs": f}).wait_recv()
        remote(w_block(f), w_block(f), wzs.at[k], wzr.at[k], {"fs": f}).wait_recv()
        for j in range(1, tp):
            tx_copy(k, j).start()

    def tokens_here():
        for k in range(fs):
            f = fs_from(k)
            for j in range(1, tp):
                t = lax.rem(me_t + tp - j, tp)
                remote(x_block(f, t), x_block(f, t), txs.at[k, j], txr.at[k, j], {"tp": t}).wait_recv()

    def experts_of(h, todo):
        def one(n, carry):
            for i, act in enumerate(todo):
                pl.when(n == i * half // len(todo))(act)
            e = h * half + n

            def block(r, carry):
                at = pl.ds(pl.multiple_of(r * tile, tile), tile)
                xs = x[at, :]
                pre_gate = jnp.dot(xs, g_out[e], preferred_element_type=f32) * depth ** (-0.5)
                pre_up = jnp.dot(xs, u_out[e], preferred_element_type=f32) * depth ** (-0.5)
                ws = jnp.transpose(w[:, at])
                lane = lax.broadcasted_iota(jnp.int32, ws.shape, 1)
                weight = jnp.sum(jnp.where(lane == e, ws, 0.0), axis=1, keepdims=True)
                value = pre_gate / (1.0 + jnp.exp(-pre_gate)) * pre_up * weight
                hid[e, at, :] = value.astype(bf16)
                return carry

            lax.fori_loop(0, total // tile, block, 0)
            return carry

        lax.fori_loop(0, half, one, 0)

    size = sub if apart else max(128, rows)
    per_owner = quarter // size
    blocks = []

    def partial_copy(ci):
        at, owner, p, slot_of, _ = blocks[ci]
        return remote(
            x.at[:, pl.ds(at, size)],
            yr.at[slot_of, :, pl.ds(pl.multiple_of(p * size, size), size)],
            ps.at[ci], pr.at[slot_of, p], {"tp": owner},
        )

    def compute(ats):
        ats = [pl.multiple_of(at, size) for at in ats]

        def block(r, carry):
            here = pl.ds(pl.multiple_of(r * tile, tile), tile)
            acc = jnp.zeros((tile, size * len(ats)), f32)
            for e in range(local):
                cols = [d_out[e, pl.ds(at, size), :] for at in ats]
                cols = cols[0] if len(cols) == 1 else jnp.concatenate(cols, axis=0)
                acc += lax.dot_general(
                    hid[e, here, :], cols, (((1,), (1,)), ((), ())), preferred_element_type=f32
                )
            acc = (acc * hidden_all ** (-0.5)).astype(bf16)
            for n, at in enumerate(ats):
                x[here, pl.ds(at, size)] = acc[:, n * size : (n + 1) * size]
            return carry

        lax.fori_loop(0, total // tile, block, 0)
        for at in ats:
            owner = at // quarter
            turn = lax.rem(me_t + tp - owner, tp)
            ci = len(blocks)
            blocks.append((at, owner, lax.rem(at, quarter) // size, lax.rem(turn + tp - 1, tp), turn != 0))

            @pl.when(turn != 0)
            def _(ci=ci):
                partial_copy(ci).start()

    def part(p):
        return pl.ds(pl.multiple_of(p * size, size), size)

    def answer_copy(k, p):
        f = fs_at(k)
        at = pl.ds(pl.multiple_of(f * cap, cap), cap)
        return remote(
            ys.at[at, part(p)], ans.at[me_f, :, part(p)], rs.at[k, p], rr.at[k, p], {"fs": f}
        )

    def finish(ci):
        here, owner, p, _, away = blocks[ci]

        @pl.when(jnp.logical_not(away))
        def _():
            for j in range(1, tp):
                ref = yr.at[j - 1, :, part(p)]
                remote(
                    ref, ref, ps.at[ci], pr.at[j - 1, p], {"tp": lax.rem(me_t + j, tp)}
                ).wait_recv()
            for k in list(range(1, fs)) + [0]:
                at = pl.ds(pl.multiple_of(fs_at(k) * cap, cap), cap)
                value = x[at, pl.ds(here, size)].astype(f32)
                for j in range(tp - 1):
                    value += yr[j, at, part(p)].astype(f32)
                if k > 0:
                    ys[at, part(p)] = value.astype(bf16)
                    answer_copy(k, p).start()
                else:
                    ans[me_f, :, part(p)] = value.astype(bf16)

    def act(f, *args):
        return lambda: f(*args)

    for s in (0, 1):
        for k in hearing:
            forward(s, k)
    for k in range(1, fs):
        tokens_on(k)
    send_gr(3, 0)
    tokens_here()
    for s in (0, 1):
        for k in range(fs):
            arrived_gr(s, k)
    experts_of(0, [act(forward, 2, k) for k in hearing])
    send_gr(4, 0)
    for k in hearing:
        forward(3, k)
    send_gr(5, 0)
    for s in (2, 3):
        for k in range(fs):
            arrived_gr(s, k)
    experts_of(1, [act(forward, 4, k) for k in hearing])
    for k in range(fs):
        for j in range(1, tp):
            tx_copy(k, j).wait_send()
    if apart:
        def pair(r, k):
            arrived_gr(4 + r, k)
            compute([(g * fs + fs_from(k)) * rows + r * sub for g in range(gr)])

        done = 0
        for r in range(split):
            order = [0] + hearing
            for n, k in enumerate(order):
                if r == split - 1 and k != 0:
                    forward(5, k)
                pair(r, k)
                while done < len(blocks) - gr:
                    finish(done)
                    done += 1
        while done < len(blocks):
            finish(done)
            done += 1
    else:
        for k in hearing:
            forward(5, k)
        for s in (4, 5):
            for k in range(fs):
                arrived_gr(s, k)
        for index in range(depth // size):
            compute([jnp.int32(index * size)])
            if index >= 1:
                finish(index - 1)
        finish(len(blocks) - 1)

    for p in range(per_owner):
        for k in range(1, fs):
            answer_copy(k, p).wait_send()
            f = fs_from(k)
            ref = ans.at[f, :, part(p)]
            remote(ref, ref, rs.at[k, p], rr.at[k, p], {"fs": f}).wait_recv()
    for k in range(1, fs):
        tok_copy(k).wait_send()
        w_copy(k).wait_send()
    for s in range(PIECES):
        for q in range(len(parts(s))):
            for k in range(fs):
                if k > 0:
                    z_copy(s, k, q).wait_send()
                for j in range(1, gr):
                    v_copy(s, k, j, q).wait_send()
    for ci in range(len(blocks)):
        @pl.when(blocks[ci][4])
        def _(ci=ci):
            partial_copy(ci).wait_send()


def place_kernel(dims, g_in, u_in, d_in, ans, slot, g_out, u_out, d_out, blended, sems):
    groups, fs, cap, tokens = dims
    f32, bf16 = jnp.float32, jnp.bfloat16
    pairs = ((g_in, g_out), (u_in, u_out), (d_in, d_out))

    def copies():
        return [
            pltpu.make_async_copy(a.at[e], b.at[e], sems.at[m, e])
            for m, (a, b) in enumerate(pairs)
            for e in range(a.shape[0])
        ]

    for c in copies():
        c.start()
    flat = (tokens, tokens)
    diagonal = lax.broadcasted_iota(jnp.int32, flat, 0) == lax.broadcasted_iota(jnp.int32, flat, 1)
    column = jnp.sum(jnp.where(diagonal, slot[...].astype(f32), 0.0), axis=1, keepdims=True)
    column = column.astype(jnp.int32)
    total = jnp.zeros(blended.shape, f32)
    each = fs // groups
    for g in range(groups):
        spots = lax.broadcasted_iota(jnp.int32, (tokens, cap), 1) + g * cap
        back = jnp.where(spots == column, 1.0, 0.0).astype(bf16)
        value = ans[g * each]
        if each > 1:
            value = value.astype(f32)
            for n in range(1, each):
                value += ans[g * each + n].astype(f32)
            value = value.astype(bf16)
        total += jnp.dot(back, value, preferred_element_type=f32)
    blended[...] = total.astype(bf16)
    for c in copies():
        c.wait()


def per_device(prompt, norm_gain, gate_master, up_master, down_master, routes, route_weights):
    gr, fs, tp = lax.axis_size("gr"), lax.axis_size("fs"), lax.axis_size("tp")
    experts, rows, width = gate_master.shape
    tokens, depth = prompt.shape
    local = experts // fs
    half = local // 2
    groups = experts // GROUP
    cap = tokens // 2
    quarter = depth // tp
    total = fs * cap
    split = 2 if rows % 256 == 0 else 1
    sub = rows // split
    size = sub if sub % 128 == 0 else max(128, rows)
    per_owner = quarter // size
    wide = max(8, local)
    bf16, f32 = jnp.bfloat16, jnp.float32
    dims = (gr, fs, tp, experts, rows, width, cap, depth, width * tp, split)
    any_spec = pl.BlockSpec(memory_space=pl.ANY)
    vmem_spec = pl.BlockSpec(memory_space=pltpu.VMEM)
    ready = (local, gr * fs * rows, width)
    dma = pltpu.SemaphoreType.DMA
    vmem = pltpu.VMEM
    n_parts = max(4, split)
    landed = 2 * (3 * ready[0] * ready[1] * ready[2] + fs * cap * quarter)
    gate_here, up_here, down_here, answers, slot = pl.pallas_call(
        functools.partial(kernel, dims),
        name="reshard_experts",
        out_shape=(
            vmem(ready, bf16), vmem(ready, bf16), vmem(ready, bf16),
            vmem((fs, cap, quarter), bf16), vmem((1, tokens), jnp.int32),
        ),
        in_specs=[vmem_spec] * 3 + [any_spec] * 4,
        out_specs=(vmem_spec,) * 5,
        scratch_shapes=[
            vmem((SLOTS, half * split, sub, width), f32),
            vmem((PIECES, fs - 1, half * split, sub, width), bf16),
            vmem((total, depth), bf16),
            vmem((wide, total), f32),
            vmem((tokens, depth), bf16),
            vmem((tokens, quarter), bf16),
            vmem((groups, cap, quarter), bf16),
            vmem((fs, wide, cap), f32),
            vmem((rows, 128), f32),
            vmem((local, total, width), bf16),
            vmem((tp - 1, total, quarter), bf16),
            vmem((total, quarter), bf16),
            dma((SLOTS, split)),
            dma((PIECES, fs, n_parts)), dma((PIECES, fs, n_parts)),
            dma((PIECES, fs, gr - 1, n_parts)), dma((PIECES, fs, gr - 1, n_parts)),
            dma((fs,)), dma((fs,)), dma((fs,)), dma((fs,)),
            dma((fs, tp)), dma((fs, tp)),
            dma((2,)),
            dma((tp * per_owner,)), dma((tp - 1, per_owner)),
            dma((fs, per_owner)), dma((fs, per_owner)),
        ],
        compiler_params=pltpu.CompilerParams(
            collective_id=0, has_side_effects=True, vmem_limit_bytes=66000000 - landed
        ),
    )(norm_gain[None, :], routes.T, route_weights.T, prompt, gate_master, up_master, down_master)
    out = jax.ShapeDtypeStruct(ready, bf16)
    return pl.pallas_call(
        functools.partial(place_kernel, (groups, fs, cap, tokens)),
        name="place_outputs",
        out_shape=(out, out, out, jax.ShapeDtypeStruct((tokens, quarter), bf16)),
        in_specs=[vmem_spec] * 5,
        out_specs=(any_spec, any_spec, any_spec, vmem_spec),
        scratch_shapes=[dma((3, local))],
        compiler_params=pltpu.CompilerParams(vmem_limit_bytes=12000000),
    )(gate_here, up_here, down_here, answers, slot)


def solution(mesh):
    both = ("gr", "fs")
    in_specs = (
        P(both, None),
        P(both),
        P(None, both, "tp"),
        P(None, both, "tp"),
        P(None, both, "tp"),
        P(both, None),
        P(both, None),
    )
    out_specs = (
        P("fs", None, "tp"),
        P("fs", None, "tp"),
        P("fs", None, "tp"),
        P(both, "tp"),
    )
    return jax.shard_map(
        per_device, mesh=mesh, in_specs=in_specs, out_specs=out_specs, check_vma=False
    )
```

```python
import functools

import jax
import jax.numpy as jnp
from jax import lax
from jax.experimental import pallas as pl
from jax.experimental.pallas import tpu as pltpu
from jax.sharding import PartitionSpec as P

EPS = 1e-06
GROUP = 8
MESH = pl.DeviceIdType.MESH
SLOTS = 4
PIECES = 6
EARLY = 1


def kernel(
    dims, gain, routes, rw, prompt, gm, um, dm, g_out, u_out, d_out, ans, slot_out,
    stage, wb, x, w, pr_in, nq, tok, wsend, gb, hid, yr, ys,
    st_sem, zs, zr, vs, vr, tzs, tzr, wzs, wzr, txs, txr, tw_sem, ps, pr, rs, rr,
):
    gr, fs, tp, experts, rows, width, cap, depth, hidden_all, split = dims
    me_g, me_f, me_t = lax.axis_index("gr"), lax.axis_index("fs"), lax.axis_index("tp")
    bf16, f32 = jnp.bfloat16, jnp.float32
    local = experts // fs
    half = local // 2
    groups = experts // GROUP
    quarter = depth // tp
    total = fs * cap
    tokens = prompt.shape[0]
    tile = min(256, cap)
    sub = rows // split
    apart = sub % 128 == 0
    masters, outs = (gm, um, dm), (g_out, u_out, d_out)

    def fs_at(k):
        return lax.rem(me_f + k, fs)

    def fs_from(k):
        return lax.rem(me_f + fs - k, fs)

    def gr_at(j):
        return lax.rem(me_g + j, gr)

    def remote(src, dst, ssem, rsem, where):
        return pltpu.make_async_remote_copy(
            src_ref=src, dst_ref=dst, send_sem=ssem, recv_sem=rsem,
            device_id=where, device_id_type=MESH,
        )

    def matrix(s):
        return (0, 1, 0, 1, 2, 2)[s]

    def half_of(s):
        return (0, 0, 1, 1, 0, 1)[s]

    def parts(s):
        h = half_of(s)
        if s >= 4 and split > 1:
            n = max(1, local // 4)
            return [(q * n, n, q * n, h * sub, sub) for q in range(local // n)]
        return [(q * half, half, h * half, q * sub, sub) for q in range(split)]

    def region(s, g, f, q):
        _, n, e0, r0, nr = parts(s)[q]
        at = pl.multiple_of((g * fs + f) * rows + r0, nr)
        return outs[matrix(s)].at[pl.ds(e0, n), pl.ds(at, nr), :]

    def buffered(s, k, q):
        b0, n, _, _, _ = parts(s)[q]
        return wb.at[s, k - 1, pl.ds(b0, n)]

    barrier = pltpu.get_barrier_semaphore()
    for k in range(1, fs):
        pl.semaphore_signal(barrier, inc=1, device_id={"fs": fs_at(k)}, device_id_type=MESH)
    for j in range(1, gr):
        pl.semaphore_signal(barrier, inc=1, device_id={"gr": gr_at(j)}, device_id_type=MESH)
    for j in range(1, tp):
        pl.semaphore_signal(
            barrier, inc=1, device_id={"tp": lax.rem(me_t + j, tp)}, device_id_type=MESH
        )

    if fs == 4:
        ahead = 1 + 2 * (me_f // 2)
        sending = [ahead, 2, 4 - ahead]
        beside, across = 3 - 2 * lax.rem(me_f, 2), 1 + (me_f + 1) // 2
        fast, slow = [beside, across], [6 - beside - across]
        inner = jnp.logical_and(me_f > 0, me_f < fs - 1)
    else:
        sending = list(range(1, fs))
        fast, slow = sending[:-1], sending[-1:]
        inner = me_f >= 0
        across = fs - 1
    items = [(s, k) for s in range(PIECES) for k in [0] + sending]

    def load(i):
        s, k = items[i]
        first = fs_at(k) * local
        slot = i % SLOTS
        if s >= 4 and split > 1:
            cuts = [(0, local, 0, half_of(s) * sub)]
        else:
            cuts = [(q * half, half, half_of(s) * half, q * sub) for q in range(split)]
        return [
            pltpu.make_async_copy(
                masters[matrix(s)].at[pl.ds(first + e0, n), pl.ds(r0, sub)],
                stage.at[slot, pl.ds(b0, n)], st_sem.at[slot, c],
            )
            for c, (b0, n, e0, r0) in enumerate(cuts)
        ]

    for i in range(SLOTS):
        for c in load(i):
            c.start()
    prompt_copy = pltpu.make_async_copy(prompt, pr_in, tw_sem.at[0])
    prompt_copy.start()
    square = (rows, rows)
    diagonal = lax.broadcasted_iota(jnp.int32, square, 0) == lax.broadcasted_iota(jnp.int32, square, 1)
    column = jnp.sum(jnp.where(diagonal, gain[...], 0.0), axis=1, keepdims=True)
    gb[...] = jnp.broadcast_to(column, gb.shape)
    pl.semaphore_wait(barrier, (fs - 1) + (gr - 1) + (tp - 1))

    def z_copy(s, k, q):
        return remote(
            buffered(s, k, q), region(s, me_g, me_f, q), zs.at[s, k, q], zr.at[s, k, q],
            {"fs": fs_at(k)},
        )

    def z_landed(s, k, q):
        f = fs_from(k)
        ref = region(s, me_g, f, q)
        return remote(ref, ref, zs.at[s, k, q], zr.at[s, k, q], {"fs": f})

    def v_copy(s, k, j, q):
        ref = region(s, me_g, fs_from(k), q)
        return remote(ref, ref, vs.at[s, k, j - 1, q], vr.at[s, k, j - 1, q], {"gr": gr_at(j)})

    def v_landed(s, k, j, q):
        g = lax.rem(me_g + gr - j, gr)
        ref = region(s, g, fs_from(k), q)
        return remote(ref, ref, vs.at[s, k, j - 1, q], vr.at[s, k, j - 1, q], {"gr": g})

    def z_send(s, k):
        for q in range(len(parts(s))):
            z_copy(s, k, q).start()

    def z_sends(s):
        for k in sending:
            z_send(s, k)

    def send_gr(s, k):
        for q in range(len(parts(s))):
            for j in range(1, gr):
                v_copy(s, k, j, q).start()

    def forward(s, k, only=None):
        for q in range(len(parts(s))) if only is None else [only]:
            z_landed(s, k, q).wait_recv()
            for j in range(1, gr):
                v_copy(s, k, j, q).start()

    def arrived_gr(s, k):
        for q in range(len(parts(s))):
            for j in range(1, gr):
                v_landed(s, k, j, q).wait_recv()

    def cast_item(i):
        s, k = items[i]
        m, h, slot = matrix(s), half_of(s), i % SLOTS
        own = isinstance(k, int) and k == 0
        for c in load(i):
            c.wait()
        base = (me_g * fs + me_f) * rows
        if s >= 4 and split > 1:
            cuts = [(0, local, 0, h * sub)]
        else:
            cuts = [(q * half, half, h * half, q * sub) for q in range(split)]
        for b0, n, e0, r0 in cuts:
            scale = None
            if m < 2:
                scale = jnp.concatenate([gb[pl.ds(r0, sub)]] * (width // 128), axis=1)

            def cast(e, carry, b0=b0, e0=e0, r0=r0, scale=scale):
                value = stage[slot, b0 + e]
                if scale is not None:
                    value = scale * value
                if own:
                    at = pl.multiple_of(base + r0, sub)
                    outs[m][e0 + e, pl.ds(at, sub), :] = value.astype(bf16)
                else:
                    wb[s, k - 1, b0 + e] = value.astype(bf16)
                return carry

            lax.fori_loop(0, n, cast, 0)
        if i + SLOTS < len(items):
            for c in load(i + SLOTS):
                c.start()
        if own:
            if s < 4:
                send_gr(s, 0)
        elif s < 4:
            z_send(s, k)
        else:
            pl.when(inner)(lambda: z_send(s, k))

    def x_block(f, t):
        return x.at[
            pl.ds(pl.multiple_of(f * cap, cap), cap),
            pl.ds(pl.multiple_of(t * quarter, quarter), quarter),
        ]

    def w_block(f):
        return w.at[:, pl.ds(pl.multiple_of(f * cap, cap), cap)]

    def tok_copy(k):
        dst = fs_at(k)
        return remote(tok.at[(dst * local) // GROUP], x_block(me_f, me_t), tzs.at[k], tzr.at[k], {"fs": dst})

    def w_copy(k):
        dst = fs_at(k)
        return remote(wsend.at[dst], w_block(me_f), wzs.at[k], wzr.at[k], {"fs": dst})

    def tx_copy(k, j):
        ref = x_block(fs_from(k), me_t)
        return remote(ref, ref, txs.at[k, j], txr.at[k, j], {"tp": lax.rem(me_t + j, tp)})

    def prepare():
        prompt_copy.wait()
        step = min(64, tokens)
        mine = pl.ds(pl.multiple_of(me_t * quarter, quarter), quarter)

        def norm(r, carry):
            at = pl.ds(pl.multiple_of(r * step, step), step)
            wide = pr_in[at, :].astype(f32)
            scale = lax.rsqrt(jnp.mean(wide * wide, axis=-1, keepdims=True) + EPS)
            nq[at, :] = (pr_in[at, mine].astype(f32) * scale).astype(bf16)
            return carry

        lax.fori_loop(0, tokens // step, norm, 0)
        first, second = routes[0:1, :], routes[1:2, :]
        pad = max(8, groups)
        low = GROUP * lax.broadcasted_iota(jnp.int32, (pad, tokens), 0)
        hits = jnp.logical_and(first >= low, first < low + GROUP)
        flat = (tokens, tokens)
        before = lax.broadcasted_iota(jnp.int32, flat, 0) < lax.broadcasted_iota(jnp.int32, flat, 1)
        counts = jnp.dot(
            jnp.where(hits, 1.0, 0.0).astype(bf16), jnp.where(before, 1.0, 0.0).astype(bf16),
            preferred_element_type=f32,
        )
        lead = (lax.broadcasted_iota(jnp.int32, (pad, tokens), 0) * cap).astype(f32)
        slot = jnp.sum(jnp.where(hits, counts + lead, 0.0), axis=0, keepdims=True).astype(jnp.int32)
        slot_out[...] = slot
        for g in range(groups):
            spots = lax.broadcasted_iota(jnp.int32, (cap, tokens), 0) + g * cap
            place = jnp.where(spots == slot, 1.0, 0.0).astype(bf16)
            packed = jnp.dot(place, nq[...], preferred_element_type=f32).astype(bf16)
            tok[g] = packed

            @pl.when((me_f * local) // GROUP == g)
            def _(packed=packed):
                x[pl.ds(pl.multiple_of(me_f * cap, cap), cap), mine] = packed

            for d in range(fs):
                if (d * local) // GROUP != g:
                    continue
                named = lax.broadcasted_iota(jnp.int32, (w.shape[0], tokens), 0) + d * local
                spread = jnp.where(first == named, rw[0:1, :], 0.0)
                spread += jnp.where(second == named, rw[1:2, :], 0.0)
                packed_w = jnp.zeros((w.shape[0], cap), f32)
                for _ in range(3):
                    top = spread.astype(bf16)
                    packed_w += lax.dot_general(
                        top, place, (((1,), (1,)), ((), ())), preferred_element_type=f32
                    )
                    spread = spread - top.astype(f32)
                wsend[d] = packed_w

                @pl.when(me_f == d)
                def _(packed_w=packed_w):
                    w[:, pl.ds(pl.multiple_of(me_f * cap, cap), cap)] = packed_w

        for k in range(1, fs):
            tok_copy(k).start()
            w_copy(k).start()
        for j in range(1, tp):
            tx_copy(0, j).start()

    per = len(items) // PIECES
    for i in range(EARLY * per):
        cast_item(i)
    prepare()
    for i in range(EARLY * per, len(items)):
        cast_item(i)

    def tokens_on(k):
        f = fs_from(k)
        remote(x_block(f, me_t), x_block(f, me_t), tzs.at[k], tzr.at[k], {"fs": f}).wait_recv()
        remote(w_block(f), w_block(f), wzs.at[k], wzr.at[k], {"fs": f}).wait_recv()
        for j in range(1, tp):
            tx_copy(k, j).start()

    def tokens_here():
        for k in range(fs):
            f = fs_from(k)
            for j in range(1, tp):
                t = lax.rem(me_t + tp - j, tp)
                remote(x_block(f, t), x_block(f, t), txs.at[k, j], txr.at[k, j], {"tp": t}).wait_recv()

    def experts_of(h, todo):
        def one(n, carry):
            for i, act in enumerate(todo):
                pl.when(n == (i + 1) * half // (len(todo) + 1))(act)
            e = h * half + n

            def block(r, carry):
                at = pl.ds(pl.multiple_of(r * tile, tile), tile)
                xs = x[at, :]
                pre_gate = jnp.dot(xs, g_out[e], preferred_element_type=f32) * depth ** (-0.5)
                pre_up = jnp.dot(xs, u_out[e], preferred_element_type=f32) * depth ** (-0.5)
                ws = jnp.transpose(w[:, at])
                lane = lax.broadcasted_iota(jnp.int32, ws.shape, 1)
                weight = jnp.sum(jnp.where(lane == e, ws, 0.0), axis=1, keepdims=True)
                value = pre_gate / (1.0 + jnp.exp(-pre_gate)) * pre_up * weight
                hid[e, at, :] = value.astype(bf16)
                return carry

            lax.fori_loop(0, total // tile, block, 0)
            return carry

        lax.fori_loop(0, half, one, 0)

    size = sub if apart else max(128, rows)
    per_owner = quarter // size
    blocks = []

    def partial_copy(ci, f):
        at, owner, p, slot_of, _ = blocks[ci]
        here = pl.ds(pl.multiple_of(f * cap, cap), cap)
        return remote(
            x.at[here, pl.ds(at, size)],
            yr.at[slot_of, here, pl.ds(pl.multiple_of(p * size, size), size)],
            ps.at[ci, f], pr.at[slot_of, p, f], {"tp": owner},
        )

    def compute(ats):
        ats = [pl.multiple_of(at, size) for at in ats]

        mine = list(range(len(blocks), len(blocks) + len(ats)))
        for at in ats:
            owner = at // quarter
            turn = lax.rem(me_t + tp - owner, tp)
            blocks.append((at, owner, lax.rem(at, quarter) // size, lax.rem(turn + tp - 1, tp), turn != 0))

        def block(i, carry):
            f = fs_at(i + 1)
            for step in range(cap // tile):
                here = pl.ds(pl.multiple_of(f * cap + step * tile, tile), tile)
                acc = jnp.zeros((tile, size * len(ats)), f32)
                for e in range(local):
                    cols = [d_out[e, pl.ds(at, size), :] for at in ats]
                    cols = cols[0] if len(cols) == 1 else jnp.concatenate(cols, axis=0)
                    acc += lax.dot_general(
                        hid[e, here, :], cols, (((1,), (1,)), ((), ())), preferred_element_type=f32
                    )
                acc = (acc * hidden_all ** (-0.5)).astype(bf16)
                for n, at in enumerate(ats):
                    x[here, pl.ds(at, size)] = acc[:, n * size : (n + 1) * size]
            for ci in mine:
                pl.when(blocks[ci][4])(lambda ci=ci: partial_copy(ci, f).start())
            return carry

        lax.fori_loop(0, fs, block, 0)

    def part(p):
        return pl.ds(pl.multiple_of(p * size, size), size)

    def answer_copy(k, p):
        f = fs_at(k)
        at = pl.ds(pl.multiple_of(f * cap, cap), cap)
        return remote(
            ys.at[at, part(p)], ans.at[me_f, :, part(p)], rs.at[k, p], rr.at[k, p], {"fs": f}
        )

    def finish(ci):
        here, owner, p, _, away = blocks[ci]

        @pl.when(jnp.logical_not(away))
        def _():
            for k in list(range(1, fs)) + [0]:
                f = fs_at(k)
                at = pl.ds(pl.multiple_of(f * cap, cap), cap)
                for j in range(1, tp):
                    ref = yr.at[j - 1, at, part(p)]
                    remote(
                        ref, ref, ps.at[ci, f], pr.at[j - 1, p, f], {"tp": lax.rem(me_t + j, tp)}
                    ).wait_recv()
                value = x[at, pl.ds(here, size)].astype(f32)
                for j in range(tp - 1):
                    value += yr[j, at, part(p)].astype(f32)
                if k > 0:
                    ys[at, part(p)] = value.astype(bf16)
                    answer_copy(k, p).start()
                else:
                    ans[me_f, :, part(p)] = value.astype(bf16)

    def act(f, *args):
        return lambda: f(*args)

    def forwards(s, ks):
        for k in ks:
            forward(s, k)

    def arrived(*steps):
        for s in steps:
            for k in range(fs):
                arrived_gr(s, k)

    forwards(0, fast)
    for k in fast:
        tokens_on(k)
    forwards(0, slow)
    forwards(1, fast)
    for k in slow:
        tokens_on(k)
    forwards(2, fast)
    send_gr(4, 0)
    forwards(3, fast)
    send_gr(5, 0)
    outer = jnp.logical_not(inner)
    forwards(1, slow)
    forwards(2, slow)
    tokens_here()
    arrived(0, 1)
    experts_of(0, [])
    forwards(3, slow)
    arrived(2, 3)

    def release(s):
        @pl.when(outer)
        def _():
            for k in slow:
                forward(s, k, 0)
            z_sends(s)

    def rest(s, k):
        for q in range(1, len(parts(s))):
            forward(s, k, q)

    if fs == 4:
        soon = [jnp.where(inner, slow[0], beside), jnp.where(inner, beside, slow[0])]
    else:
        soon = list(range(1, fs - 1))
    late = across

    experts_of(1, [act(forward, 4, soon[0]), act(release, 4)])
    for k in range(fs):
        for j in range(1, tp):
            tx_copy(k, j).wait_send()
    if apart:
        def pair(r, k):
            arrived_gr(4 + r, k)
            compute([(g * fs + fs_from(k)) * rows + r * sub for g in range(gr)])

        done = [0]

        def finish_to(count):
            while done[0] < count:
                finish(done[0])
                done[0] += 1

        def step(r, k, lag=2 * gr):
            pair(r, k)
            finish_to(len(blocks) - lag)

        count = len(parts(5))
        step(0, 0)
        pl.when(inner)(lambda: forward(4, soon[-1], 0))
        rest(4, soon[-1])
        for k in soon[1:-1]:
            forward(4, k)
        step(0, soon[0])
        for q in range(count // 2):
            forward(4, late, q)
        for k in soon[1:]:
            step(0, k)
        for q in range(count // 2, count):
            forward(4, late, q)
        pl.when(outer)(lambda: forward(5, soon[0]))
        step(0, late)
        step(1, 0)
        release(5)
        pl.when(inner)(lambda: forward(5, soon[0]))
        step(1, soon[0], gr)
        pl.when(inner)(lambda: forward(5, soon[-1], 0))
        rest(5, soon[-1])
        for k in soon[1:-1]:
            forward(5, k)
        for q in range(count - 2):
            forward(5, late, q)
        for k in soon[1:]:
            step(1, k, gr)
        for q in range(count - 2, count):
            forward(5, late, q)
        step(1, late, gr)
        finish_to(len(blocks))
    else:
        forwards(4, soon[1:] + [late])
        forwards(5, soon + [late])
        for s in (4, 5):
            for k in range(fs):
                arrived_gr(s, k)
        for index in range(depth // size):
            compute([jnp.int32(index * size)])
            if index >= 1:
                finish(index - 1)
        finish(len(blocks) - 1)

    for p in range(per_owner):
        for k in range(1, fs):
            answer_copy(k, p).wait_send()
            f = fs_from(k)
            ref = ans.at[f, :, part(p)]
            remote(ref, ref, rs.at[k, p], rr.at[k, p], {"fs": f}).wait_recv()
    for k in range(1, fs):
        tok_copy(k).wait_send()
        w_copy(k).wait_send()
    for s in range(PIECES):
        for q in range(len(parts(s))):
            for k in range(fs):
                if k > 0:
                    z_copy(s, k, q).wait_send()
                for j in range(1, gr):
                    v_copy(s, k, j, q).wait_send()
    for ci in range(len(blocks)):
        @pl.when(blocks[ci][4])
        def _(ci=ci):
            for f in range(fs):
                partial_copy(ci, f).wait_send()


def place_kernel(dims, g_in, u_in, d_in, ans, slot, g_out, u_out, d_out, blended, sems):
    groups, fs, cap, tokens = dims
    f32, bf16 = jnp.float32, jnp.bfloat16
    pairs = ((g_in, g_out), (u_in, u_out), (d_in, d_out))

    def copies():
        return [
            pltpu.make_async_copy(a.at[e], b.at[e], sems.at[m, e])
            for m, (a, b) in enumerate(pairs)
            for e in range(a.shape[0])
        ]

    for c in copies():
        c.start()
    flat = (tokens, tokens)
    diagonal = lax.broadcasted_iota(jnp.int32, flat, 0) == lax.broadcasted_iota(jnp.int32, flat, 1)
    column = jnp.sum(jnp.where(diagonal, slot[...].astype(f32), 0.0), axis=1, keepdims=True)
    column = column.astype(jnp.int32)
    total = jnp.zeros(blended.shape, f32)
    each = fs // groups
    for g in range(groups):
        spots = lax.broadcasted_iota(jnp.int32, (tokens, cap), 1) + g * cap
        back = jnp.where(spots == column, 1.0, 0.0).astype(bf16)
        value = ans[g * each]
        if each > 1:
            value = value.astype(f32)
            for n in range(1, each):
                value += ans[g * each + n].astype(f32)
            value = value.astype(bf16)
        total += jnp.dot(back, value, preferred_element_type=f32)
    blended[...] = total.astype(bf16)
    for c in copies():
        c.wait()


def per_device(prompt, norm_gain, gate_master, up_master, down_master, routes, route_weights):
    gr, fs, tp = lax.axis_size("gr"), lax.axis_size("fs"), lax.axis_size("tp")
    experts, rows, width = gate_master.shape
    tokens, depth = prompt.shape
    local = experts // fs
    half = local // 2
    groups = experts // GROUP
    cap = tokens // 2
    quarter = depth // tp
    total = fs * cap
    split = 2 if rows % 256 == 0 else 1
    sub = rows // split
    size = sub if sub % 128 == 0 else max(128, rows)
    per_owner = quarter // size
    wide = max(8, local)
    bf16, f32 = jnp.bfloat16, jnp.float32
    dims = (gr, fs, tp, experts, rows, width, cap, depth, width * tp, split)
    any_spec = pl.BlockSpec(memory_space=pl.ANY)
    vmem_spec = pl.BlockSpec(memory_space=pltpu.VMEM)
    ready = (local, gr * fs * rows, width)
    dma = pltpu.SemaphoreType.DMA
    vmem = pltpu.VMEM
    n_parts = max(4, split)
    landed = 2 * (3 * ready[0] * ready[1] * ready[2] + fs * cap * quarter)
    gate_here, up_here, down_here, answers, slot = pl.pallas_call(
        functools.partial(kernel, dims),
        name="reshard_experts",
        out_shape=(
            vmem(ready, bf16), vmem(ready, bf16), vmem(ready, bf16),
            vmem((fs, cap, quarter), bf16), vmem((1, tokens), jnp.int32),
        ),
        in_specs=[vmem_spec] * 3 + [any_spec] * 4,
        out_specs=(vmem_spec,) * 5,
        scratch_shapes=[
            vmem((SLOTS, half * split, sub, width), f32),
            vmem((PIECES, fs - 1, half * split, sub, width), bf16),
            vmem((total, depth), bf16),
            vmem((wide, total), f32),
            vmem((tokens, depth), bf16),
            vmem((tokens, quarter), bf16),
            vmem((groups, cap, quarter), bf16),
            vmem((fs, wide, cap), f32),
            vmem((rows, 128), f32),
            vmem((local, total, width), bf16),
            vmem((tp - 1, total, quarter), bf16),
            vmem((total, quarter), bf16),
            dma((SLOTS, split)),
            dma((PIECES, fs, n_parts)), dma((PIECES, fs, n_parts)),
            dma((PIECES, fs, gr - 1, n_parts)), dma((PIECES, fs, gr - 1, n_parts)),
            dma((fs,)), dma((fs,)), dma((fs,)), dma((fs,)),
            dma((fs, tp)), dma((fs, tp)),
            dma((2,)),
            dma((tp * per_owner, fs)), dma((tp - 1, per_owner, fs)),
            dma((fs, per_owner)), dma((fs, per_owner)),
        ],
        compiler_params=pltpu.CompilerParams(
            collective_id=0, has_side_effects=True, vmem_limit_bytes=66000000 - landed
        ),
    )(norm_gain[None, :], routes.T, route_weights.T, prompt, gate_master, up_master, down_master)
    out = jax.ShapeDtypeStruct(ready, bf16)
    return pl.pallas_call(
        functools.partial(place_kernel, (groups, fs, cap, tokens)),
        name="place_outputs",
        out_shape=(out, out, out, jax.ShapeDtypeStruct((tokens, quarter), bf16)),
        in_specs=[vmem_spec] * 5,
        out_specs=(any_spec, any_spec, any_spec, vmem_spec),
        scratch_shapes=[dma((3, local))],
        compiler_params=pltpu.CompilerParams(vmem_limit_bytes=12000000),
    )(gate_here, up_here, down_here, answers, slot)


def solution(mesh):
    both = ("gr", "fs")
    in_specs = (
        P(both, None),
        P(both),
        P(None, both, "tp"),
        P(None, both, "tp"),
        P(None, both, "tp"),
        P(both, None),
        P(both, None),
    )
    out_specs = (
        P("fs", None, "tp"),
        P("fs", None, "tp"),
        P("fs", None, "tp"),
        P(both, "tp"),
    )
    return jax.shard_map(
        per_device, mesh=mesh, in_specs=in_specs, out_specs=out_specs, check_vma=False
    )
```

```python
import functools

import jax
import jax.numpy as jnp
from jax import lax
from jax.experimental import pallas as pl
from jax.experimental.pallas import tpu as pltpu
from jax.sharding import PartitionSpec as P

EPS = 1e-06
GROUP = 8
MESH = pl.DeviceIdType.MESH
SLOTS = 4
PIECES = 6
EARLY = 1


def kernel(
    dims, gain, routes, rw, prompt, gm, um, dm, g_out, u_out, d_out, ans, slot_out,
    stage, wb, x, w, pr_in, nq, tok, wsend, gb, hid, yr, ys,
    st_sem, zs, zr, zl, vs, vr, tzs, tzr, wzs, wzr, txs, txr, tw_sem, ps, pr, rs, rr,
):
    gr, fs, tp, experts, rows, width, cap, depth, hidden_all, split = dims
    me_g, me_f, me_t = lax.axis_index("gr"), lax.axis_index("fs"), lax.axis_index("tp")
    bf16, f32 = jnp.bfloat16, jnp.float32
    local = experts // fs
    half = local // 2
    groups = experts // GROUP
    quarter = depth // tp
    total = fs * cap
    tokens = prompt.shape[0]
    tile = min(256, cap)
    sub = rows // split
    apart = sub % 128 == 0
    masters, outs = (gm, um, dm), (g_out, u_out, d_out)

    def fs_at(k):
        return lax.rem(me_f + k, fs)

    def fs_from(k):
        return lax.rem(me_f + fs - k, fs)

    def gr_at(j):
        return lax.rem(me_g + j, gr)

    def remote(src, dst, ssem, rsem, where):
        return pltpu.make_async_remote_copy(
            src_ref=src, dst_ref=dst, send_sem=ssem, recv_sem=rsem,
            device_id=where, device_id_type=MESH,
        )

    def matrix(s):
        return (0, 1, 0, 1, 2, 2)[s]

    def half_of(s):
        return (0, 0, 1, 1, 0, 1)[s]

    def parts(s):
        h = half_of(s)
        if s >= 4 and split > 1:
            n = max(1, local // 4)
            return [(q * n, n, q * n, h * sub, sub) for q in range(local // n)]
        return [(q * half, half, h * half, q * sub, sub) for q in range(split)]

    def region(s, g, f, q):
        _, n, e0, r0, nr = parts(s)[q]
        at = pl.multiple_of((g * fs + f) * rows + r0, nr)
        return outs[matrix(s)].at[pl.ds(e0, n), pl.ds(at, nr), :]

    def buffered(s, k, q):
        b0, n, _, _, _ = parts(s)[q]
        return wb.at[s, k - 1, pl.ds(b0, n)]

    barrier = pltpu.get_barrier_semaphore()
    for k in range(1, fs):
        pl.semaphore_signal(barrier, inc=1, device_id={"fs": fs_at(k)}, device_id_type=MESH)
    for j in range(1, gr):
        pl.semaphore_signal(barrier, inc=1, device_id={"gr": gr_at(j)}, device_id_type=MESH)
    for j in range(1, tp):
        pl.semaphore_signal(
            barrier, inc=1, device_id={"tp": lax.rem(me_t + j, tp)}, device_id_type=MESH
        )

    if fs == 4:
        ahead = 1 + 2 * (me_f // 2)
        sending = [ahead, 2, 4 - ahead]
        beside, across = 3 - 2 * lax.rem(me_f, 2), 1 + (me_f + 1) // 2
        fast, slow = [beside, across], [6 - beside - across]
        inner = jnp.logical_and(me_f > 0, me_f < fs - 1)
    else:
        sending = list(range(1, fs))
        fast, slow = sending[:-1], sending[-1:]
        inner = me_f >= 0
        across = fs - 1
    items = [(s, k) for s in range(PIECES) for k in [0] + sending]

    def load(i):
        s, k = items[i]
        first = fs_at(k) * local
        slot = i % SLOTS
        if s >= 4 and split > 1:
            cuts = [(0, local, 0, half_of(s) * sub)]
        else:
            cuts = [(q * half, half, half_of(s) * half, q * sub) for q in range(split)]
        return [
            pltpu.make_async_copy(
                masters[matrix(s)].at[pl.ds(first + e0, n), pl.ds(r0, sub)],
                stage.at[slot, pl.ds(b0, n)], st_sem.at[slot, c],
            )
            for c, (b0, n, e0, r0) in enumerate(cuts)
        ]

    for i in range(SLOTS):
        for c in load(i):
            c.start()
    prompt_copy = pltpu.make_async_copy(prompt, pr_in, tw_sem.at[0])
    prompt_copy.start()
    square = (rows, rows)
    diagonal = lax.broadcasted_iota(jnp.int32, square, 0) == lax.broadcasted_iota(jnp.int32, square, 1)
    column = jnp.sum(jnp.where(diagonal, gain[...], 0.0), axis=1, keepdims=True)
    gb[...] = jnp.broadcast_to(column, gb.shape)
    pl.semaphore_wait(barrier, (fs - 1) + (gr - 1) + (tp - 1))

    def z_sem(s, k, q):
        return zl.at[s - 4, k - 1, q] if s >= 4 else zr.at[s, k - 1]

    def piece(s, g, f):
        h = half_of(s)
        e0, n, r0, nr = (0, local, h * sub, sub) if s >= 4 and split > 1 else (h * half, half, 0, rows)
        at = pl.multiple_of((g * fs + f) * rows + r0, nr)
        return outs[matrix(s)].at[pl.ds(e0, n), pl.ds(at, nr), :]

    def z_copy(s, k, q):
        return remote(
            buffered(s, k, q), region(s, me_g, me_f, q), zs.at[s], z_sem(s, k, q), {"fs": fs_at(k)},
        )

    def z_landed(s, k, q):
        f = fs_from(k)
        ref = piece(s, me_g, f) if s < 4 else region(s, me_g, f, q)
        return remote(ref, ref, zs.at[s], z_sem(s, k, q), {"fs": f})

    def v_copy(s, k, j, q):
        ref = region(s, me_g, fs_from(k), q)
        return remote(ref, ref, vs.at[matrix(s), j - 1], vr.at[s, k, j - 1], {"gr": gr_at(j)})

    def v_landed(s, k, j):
        g = lax.rem(me_g + gr - j, gr)
        ref = piece(s, g, fs_from(k))
        return remote(ref, ref, vs.at[matrix(s), j - 1], vr.at[s, k, j - 1], {"gr": g})

    def z_send(s, k):
        for q in range(len(parts(s))):
            z_copy(s, k, q).start()

    def z_sends(s):
        for k in sending:
            z_send(s, k)

    def send_gr(s, k):
        for q in range(len(parts(s))):
            for j in range(1, gr):
                v_copy(s, k, j, q).start()

    def forward(s, k, only=None):
        for q in range(len(parts(s))) if only is None else [only]:
            if s >= 4 or q == 0:
                z_landed(s, k, q).wait_recv()
            for j in range(1, gr):
                v_copy(s, k, j, q).start()

    def arrived_gr(s, k):
        for j in range(1, gr):
            v_landed(s, k, j).wait_recv()

    def cast_item(i):
        s, k = items[i]
        m, h, slot = matrix(s), half_of(s), i % SLOTS
        own = isinstance(k, int) and k == 0
        for c in load(i):
            c.wait()
        base = (me_g * fs + me_f) * rows
        if s >= 4 and split > 1:
            cuts = [(0, local, 0, h * sub)]
        else:
            cuts = [(q * half, half, h * half, q * sub) for q in range(split)]
        for b0, n, e0, r0 in cuts:
            scale = None
            if m < 2:
                scale = jnp.concatenate([gb[pl.ds(r0, sub)]] * (width // 128), axis=1)

            def cast(e, carry, b0=b0, e0=e0, r0=r0, scale=scale):
                value = stage[slot, b0 + e]
                if scale is not None:
                    value = scale * value
                if own:
                    at = pl.multiple_of(base + r0, sub)
                    outs[m][e0 + e, pl.ds(at, sub), :] = value.astype(bf16)
                else:
                    wb[s, k - 1, b0 + e] = value.astype(bf16)
                return carry

            lax.fori_loop(0, n, cast, 0)
        if i + SLOTS < len(items):
            for c in load(i + SLOTS):
                c.start()
        if own:
            if s < 4:
                send_gr(s, 0)
        elif s < 4:
            z_send(s, k)
        else:
            pl.when(inner)(lambda: z_send(s, k))

    def x_block(f, t):
        return x.at[
            pl.ds(pl.multiple_of(f * cap, cap), cap),
            pl.ds(pl.multiple_of(t * quarter, quarter), quarter),
        ]

    def w_block(f):
        return w.at[:, pl.ds(pl.multiple_of(f * cap, cap), cap)]

    def tok_copy(k):
        dst = fs_at(k)
        return remote(tok.at[(dst * local) // GROUP], x_block(me_f, me_t), tzs.at[k], tzr.at[k], {"fs": dst})

    def w_copy(k):
        dst = fs_at(k)
        return remote(wsend.at[dst], w_block(me_f), wzs.at[k], wzr.at[k], {"fs": dst})

    def tx_copy(k, j):
        ref = x_block(fs_from(k), me_t)
        return remote(ref, ref, txs.at[j - 1], txr.at[k, j - 1], {"tp": lax.rem(me_t + j, tp)})

    def prepare():
        prompt_copy.wait()
        step = min(64, tokens)
        mine = pl.ds(pl.multiple_of(me_t * quarter, quarter), quarter)

        def norm(r, carry):
            at = pl.ds(pl.multiple_of(r * step, step), step)
            wide = pr_in[at, :].astype(f32)
            scale = lax.rsqrt(jnp.mean(wide * wide, axis=-1, keepdims=True) + EPS)
            nq[at, :] = (pr_in[at, mine].astype(f32) * scale).astype(bf16)
            return carry

        lax.fori_loop(0, tokens // step, norm, 0)
        first, second = routes[0:1, :], routes[1:2, :]
        pad = max(8, groups)
        low = GROUP * lax.broadcasted_iota(jnp.int32, (pad, tokens), 0)
        hits = jnp.logical_and(first >= low, first < low + GROUP)
        flat = (tokens, tokens)
        before = lax.broadcasted_iota(jnp.int32, flat, 0) < lax.broadcasted_iota(jnp.int32, flat, 1)
        counts = jnp.dot(
            jnp.where(hits, 1.0, 0.0).astype(bf16), jnp.where(before, 1.0, 0.0).astype(bf16),
            preferred_element_type=f32,
        )
        lead = (lax.broadcasted_iota(jnp.int32, (pad, tokens), 0) * cap).astype(f32)
        slot = jnp.sum(jnp.where(hits, counts + lead, 0.0), axis=0, keepdims=True).astype(jnp.int32)
        slot_out[...] = slot
        for g in range(groups):
            spots = lax.broadcasted_iota(jnp.int32, (cap, tokens), 0) + g * cap
            place = jnp.where(spots == slot, 1.0, 0.0).astype(bf16)
            packed = jnp.dot(place, nq[...], preferred_element_type=f32).astype(bf16)
            tok[g] = packed

            @pl.when((me_f * local) // GROUP == g)
            def _(packed=packed):
                x[pl.ds(pl.multiple_of(me_f * cap, cap), cap), mine] = packed

            for d in range(fs):
                if (d * local) // GROUP != g:
                    continue
                named = lax.broadcasted_iota(jnp.int32, (w.shape[0], tokens), 0) + d * local
                spread = jnp.where(first == named, rw[0:1, :], 0.0)
                spread += jnp.where(second == named, rw[1:2, :], 0.0)
                packed_w = jnp.zeros((w.shape[0], cap), f32)
                for _ in range(3):
                    top = spread.astype(bf16)
                    packed_w += lax.dot_general(
                        top, place, (((1,), (1,)), ((), ())), preferred_element_type=f32
                    )
                    spread = spread - top.astype(f32)
                wsend[d] = packed_w

                @pl.when(me_f == d)
                def _(packed_w=packed_w):
                    w[:, pl.ds(pl.multiple_of(me_f * cap, cap), cap)] = packed_w

        for k in range(1, fs):
            tok_copy(k).start()
            w_copy(k).start()
        for j in range(1, tp):
            tx_copy(0, j).start()

    per = len(items) // PIECES
    for i in range(EARLY * per):
        cast_item(i)
    prepare()
    for i in range(EARLY * per, len(items)):
        cast_item(i)

    def tokens_on(k):
        f = fs_from(k)
        remote(x_block(f, me_t), x_block(f, me_t), tzs.at[k], tzr.at[k], {"fs": f}).wait_recv()
        remote(w_block(f), w_block(f), wzs.at[k], wzr.at[k], {"fs": f}).wait_recv()
        for j in range(1, tp):
            tx_copy(k, j).start()

    def tokens_here():
        for k in range(fs):
            f = fs_from(k)
            for j in range(1, tp):
                t = lax.rem(me_t + tp - j, tp)
                remote(x_block(f, t), x_block(f, t), txs.at[j - 1], txr.at[k, j - 1], {"tp": t}).wait_recv()

    def experts_of(h, todo):
        def one(n, carry):
            for i, act in enumerate(todo):
                pl.when(n == (i + 1) * half // (len(todo) + 1))(act)
            e = h * half + n

            def block(r, carry):
                at = pl.ds(pl.multiple_of(r * tile, tile), tile)
                xs = x[at, :]
                pre_gate = jnp.dot(xs, g_out[e], preferred_element_type=f32) * depth ** (-0.5)
                pre_up = jnp.dot(xs, u_out[e], preferred_element_type=f32) * depth ** (-0.5)
                ws = jnp.transpose(w[:, at])
                lane = lax.broadcasted_iota(jnp.int32, ws.shape, 1)
                weight = jnp.sum(jnp.where(lane == e, ws, 0.0), axis=1, keepdims=True)
                value = pre_gate / (1.0 + jnp.exp(-pre_gate)) * pre_up * weight
                hid[e, at, :] = value.astype(bf16)
                return carry

            lax.fori_loop(0, total // tile, block, 0)
            return carry

        lax.fori_loop(0, half, one, 0)

    size = sub if apart else max(128, rows)
    per_owner = quarter // size
    blocks = []

    def partial_copy(ci, f):
        at, owner, p, slot_of, _ = blocks[ci]
        here = pl.ds(pl.multiple_of(f * cap, cap), cap)
        return remote(
            x.at[here, pl.ds(at, size)],
            yr.at[slot_of, here, pl.ds(pl.multiple_of(p * size, size), size)],
            ps.at[ci], pr.at[slot_of, p, f], {"tp": owner},
        )

    def compute(ats):
        ats = [pl.multiple_of(at, size) for at in ats]

        mine = list(range(len(blocks), len(blocks) + len(ats)))
        for at in ats:
            owner = at // quarter
            turn = lax.rem(me_t + tp - owner, tp)
            blocks.append((at, owner, lax.rem(at, quarter) // size, lax.rem(turn + tp - 1, tp), turn != 0))

        def block(i, carry):
            f = fs_at(i + 1)
            for step in range(cap // tile):
                here = pl.ds(pl.multiple_of(f * cap + step * tile, tile), tile)
                acc = jnp.zeros((tile, size * len(ats)), f32)
                for e in range(local):
                    cols = [d_out[e, pl.ds(at, size), :] for at in ats]
                    cols = cols[0] if len(cols) == 1 else jnp.concatenate(cols, axis=0)
                    acc += lax.dot_general(
                        hid[e, here, :], cols, (((1,), (1,)), ((), ())), preferred_element_type=f32
                    )
                acc = (acc * hidden_all ** (-0.5)).astype(bf16)
                for n, at in enumerate(ats):
                    x[here, pl.ds(at, size)] = acc[:, n * size : (n + 1) * size]
            for ci in mine:
                pl.when(blocks[ci][4])(lambda ci=ci: partial_copy(ci, f).start())
            return carry

        lax.fori_loop(0, fs, block, 0)

    def part(p):
        return pl.ds(pl.multiple_of(p * size, size), size)

    def answer_copy(k, p):
        f = fs_at(k)
        at = pl.ds(pl.multiple_of(f * cap, cap), cap)
        return remote(
            ys.at[at, part(p)], ans.at[me_f, :, part(p)], rs.at[k - 1], rr.at[k - 1], {"fs": f}
        )

    held = [False]

    def release_answers(count):
        held[0] = False
        for ci in range(count):
            @pl.when(jnp.logical_not(blocks[ci][4]))
            def _(ci=ci):
                for k in range(1, fs):
                    answer_copy(k, blocks[ci][2]).start()

    def finish(ci):
        here, owner, p, _, away = blocks[ci]

        @pl.when(jnp.logical_not(away))
        def _():
            for k in list(range(1, fs)) + [0]:
                f = fs_at(k)
                at = pl.ds(pl.multiple_of(f * cap, cap), cap)
                for j in range(1, tp):
                    ref = yr.at[j - 1, at, part(p)]
                    remote(
                        ref, ref, ps.at[ci], pr.at[j - 1, p, f], {"tp": lax.rem(me_t + j, tp)}
                    ).wait_recv()
                value = x[at, pl.ds(here, size)].astype(f32)
                for j in range(tp - 1):
                    value += yr[j, at, part(p)].astype(f32)
                if k > 0:
                    ys[at, part(p)] = value.astype(bf16)
                    if not held[0]:
                        answer_copy(k, p).start()
                else:
                    ans[me_f, :, part(p)] = value.astype(bf16)

    def drain(steps, gathered=()):
        for s in steps:
            remote(wb.at[s], wb.at[s], zs.at[s], zr.at[0, 0], {"fs": fs_at(1)}).wait_send()
        for m in gathered:
            ref = outs[m].at[:, pl.ds(pl.multiple_of(me_g * fs * rows, rows), fs * rows), :]
            for j in range(1, gr):
                remote(ref, ref, vs.at[m, j - 1], vr.at[0, 0, j - 1], {"gr": gr_at(j)}).wait_send()
        if 0 in steps:
            for k in range(1, fs):
                tok_copy(k).wait_send()
                w_copy(k).wait_send()

    def drain_partials(which):
        for ci in which:
            @pl.when(blocks[ci][4])
            def _(ci=ci):
                at, owner, p, slot_of, _ = blocks[ci]
                ref = x.at[:, pl.ds(at, size)]
                remote(ref, ref, ps.at[ci], pr.at[slot_of, p, 0], {"tp": owner}).wait_send()

    def act(f, *args):
        return lambda: f(*args)

    def forwards(s, ks):
        for k in ks:
            forward(s, k)

    def arrived(*steps):
        for s in steps:
            for k in range(fs):
                arrived_gr(s, k)

    forwards(0, fast)
    for k in fast:
        tokens_on(k)
    forwards(0, slow)
    forwards(1, fast)
    for k in slow:
        tokens_on(k)
    forwards(2, fast)
    send_gr(4, 0)
    forwards(3, fast)
    send_gr(5, 0)
    outer = jnp.logical_not(inner)
    forwards(1, slow)
    forwards(2, slow)
    tokens_here()
    arrived(0, 1)
    experts_of(0, [])
    forwards(3, slow)
    arrived(2, 3)

    def release(s):
        @pl.when(outer)
        def _():
            for k in slow:
                forward(s, k, 0)
            if s == 4:
                z_sends(4)
                z_send(5, sending[0])
            else:
                for k in sending[:0:-1]:
                    z_send(5, k)

    def rest(s, k):
        for q in range(1, len(parts(s))):
            forward(s, k, q)

    if fs == 4:
        soon = [jnp.where(inner, slow[0], beside), jnp.where(inner, beside, slow[0])]
    else:
        soon = list(range(1, fs - 1))
    late = across

    experts_of(1, [act(forward, 4, soon[0]), act(release, 4)])
    for j in range(1, tp):
        ref = x.at[:, pl.ds(pl.multiple_of(me_t * quarter, quarter), quarter)]
        remote(ref, ref, txs.at[j - 1], txr.at[0, j - 1], {"tp": lax.rem(me_t + j, tp)}).wait_send()
    if apart:
        def pair(r, k):
            arrived_gr(4 + r, k)
            compute([(g * fs + fs_from(k)) * rows + r * sub for g in range(gr)])

        done = [0]

        def finish_to(count):
            while done[0] < count:
                finish(done[0])
                done[0] += 1

        def step(r, k, lag=2 * gr):
            pair(r, k)
            finish_to(len(blocks) - lag)

        count = len(parts(5))
        held[0] = True
        step(0, 0)
        pl.when(inner)(lambda: forward(4, soon[-1], 0))
        rest(4, soon[-1])
        for k in soon[1:-1]:
            forward(4, k)
        step(0, soon[0])
        drain([0, 1, 2, 3])
        for q in range(count // 2):
            forward(4, late, q)
        for k in soon[1:]:
            step(0, k)
        for q in range(count // 2, count):
            forward(4, late, q)
        pl.when(outer)(lambda: forward(5, soon[0]))
        step(0, late)
        step(1, 0)
        release(5)
        pl.when(inner)(lambda: forward(5, soon[0]))
        step(1, soon[0], gr)
        middle, final = soon[1:], late
        if fs == 4:
            middle, final = [jnp.where(inner, beside, across)], jnp.where(inner, across, slow[0])
            pl.when(outer)(lambda: forward(5, slow[0], 1))
        forwards(5, middle)
        drain([4])
        drain_partials(range(gr * fs))

        @pl.when(inner)
        def _():
            for q in range(count - 2):
                forward(5, final, q)

        for k in middle:
            step(1, k, gr)
        for q in range(count - 2, count):
            forward(5, final, q)
        release_answers(done[0])
        step(1, final, gr)
        finish_to(len(blocks))
    else:
        forwards(4, soon[1:] + [late])
        forwards(5, soon + [late])
        for s in (4, 5):
            for k in range(fs):
                arrived_gr(s, k)
        for index in range(depth // size):
            compute([jnp.int32(index * size)])
            if index >= 1:
                finish(index - 1)
        finish(len(blocks) - 1)

    for k in range(1, fs):
        f = fs_at(k)
        ref = ys.at[pl.ds(pl.multiple_of(f * cap, cap), cap), :]
        remote(ref, ref, rs.at[k - 1], rr.at[k - 1], {"fs": f}).wait_send()
    drain([5] if apart else range(PIECES), range(3))
    drain_partials(range(gr * fs if apart else 0, len(blocks)))
    for k in range(1, fs):
        f = fs_from(k)
        remote(ans.at[f], ans.at[f], rs.at[k - 1], rr.at[k - 1], {"fs": f}).wait_recv()


def place_kernel(dims, g_in, u_in, d_in, ans, slot, g_out, u_out, d_out, blended, mixed, sems, mixed_sem):
    groups, fs, cap, tokens = dims
    f32, bf16 = jnp.float32, jnp.bfloat16
    pairs = ((g_in, g_out), (u_in, u_out), (d_in, d_out))

    def copies():
        return [
            pltpu.make_async_copy(a.at[e], b.at[e], sems.at[m, e])
            for m, (a, b) in enumerate(pairs)
            for e in range(a.shape[0])
        ]

    for c in copies():
        c.start()
    flat = (tokens, tokens)
    diagonal = lax.broadcasted_iota(jnp.int32, flat, 0) == lax.broadcasted_iota(jnp.int32, flat, 1)
    column = jnp.sum(jnp.where(diagonal, slot[...].astype(f32), 0.0), axis=1, keepdims=True)
    column = column.astype(jnp.int32)
    total = jnp.zeros(blended.shape, f32)
    each = fs // groups
    for g in range(groups):
        spots = lax.broadcasted_iota(jnp.int32, (tokens, cap), 1) + g * cap
        back = jnp.where(spots == column, 1.0, 0.0).astype(bf16)
        value = ans[g * each]
        if each > 1:
            value = value.astype(f32)
            for n in range(1, each):
                value += ans[g * each + n].astype(f32)
            value = value.astype(bf16)
        total += jnp.dot(back, value, preferred_element_type=f32)
    mixed[...] = total.astype(bf16)
    last = pltpu.make_async_copy(mixed, blended, mixed_sem)
    last.start()
    for c in copies():
        c.wait()
    last.wait()


def per_device(prompt, norm_gain, gate_master, up_master, down_master, routes, route_weights):
    gr, fs, tp = lax.axis_size("gr"), lax.axis_size("fs"), lax.axis_size("tp")
    experts, rows, width = gate_master.shape
    tokens, depth = prompt.shape
    local = experts // fs
    half = local // 2
    groups = experts // GROUP
    cap = tokens // 2
    quarter = depth // tp
    total = fs * cap
    split = 2 if rows % 256 == 0 else 1
    sub = rows // split
    size = sub if sub % 128 == 0 else max(128, rows)
    per_owner = quarter // size
    wide = max(8, local)
    bf16, f32 = jnp.bfloat16, jnp.float32
    dims = (gr, fs, tp, experts, rows, width, cap, depth, width * tp, split)
    any_spec = pl.BlockSpec(memory_space=pl.ANY)
    vmem_spec = pl.BlockSpec(memory_space=pltpu.VMEM)
    ready = (local, gr * fs * rows, width)
    dma = pltpu.SemaphoreType.DMA
    vmem = pltpu.VMEM
    n_parts = max(4, split)
    landed = 2 * (3 * ready[0] * ready[1] * ready[2] + fs * cap * quarter)
    gate_here, up_here, down_here, answers, slot = pl.pallas_call(
        functools.partial(kernel, dims),
        name="reshard_experts",
        out_shape=(
            vmem(ready, bf16), vmem(ready, bf16), vmem(ready, bf16),
            vmem((fs, cap, quarter), bf16), vmem((1, tokens), jnp.int32),
        ),
        in_specs=[vmem_spec] * 3 + [any_spec] * 4,
        out_specs=(vmem_spec,) * 5,
        scratch_shapes=[
            vmem((SLOTS, half * split, sub, width), f32),
            vmem((PIECES, fs - 1, half * split, sub, width), bf16),
            vmem((total, depth), bf16),
            vmem((wide, total), f32),
            vmem((tokens, depth), bf16),
            vmem((tokens, quarter), bf16),
            vmem((groups, cap, quarter), bf16),
            vmem((fs, wide, cap), f32),
            vmem((rows, 128), f32),
            vmem((local, total, width), bf16),
            vmem((tp - 1, total, quarter), bf16),
            vmem((total, quarter), bf16),
            dma((SLOTS, split)),
            dma((PIECES,)), dma((4, fs - 1)), dma((2, fs - 1, n_parts)),
            dma((3, gr - 1)), dma((PIECES, fs, gr - 1)),
            dma((fs,)), dma((fs,)), dma((fs,)), dma((fs,)),
            dma((tp - 1,)), dma((fs, tp - 1)),
            dma((1,)),
            dma((tp * per_owner,)), dma((tp - 1, per_owner, fs)),
            dma((fs - 1,)), dma((fs - 1,)),
        ],
        compiler_params=pltpu.CompilerParams(
            collective_id=0, has_side_effects=True, vmem_limit_bytes=66000000 - landed
        ),
    )(norm_gain[None, :], routes.T, route_weights.T, prompt, gate_master, up_master, down_master)
    out = jax.ShapeDtypeStruct(ready, bf16)
    return pl.pallas_call(
        functools.partial(place_kernel, (groups, fs, cap, tokens)),
        name="place_outputs",
        out_shape=(out, out, out, jax.ShapeDtypeStruct((tokens, quarter), bf16)),
        in_specs=[vmem_spec] * 5,
        out_specs=(any_spec,) * 4,
        scratch_shapes=[vmem((tokens, quarter), bf16), dma((3, local)), dma],
        compiler_params=pltpu.CompilerParams(vmem_limit_bytes=12000000),
    )(gate_here, up_here, down_here, answers, slot)


def solution(mesh):
    both = ("gr", "fs")
    in_specs = (
        P(both, None),
        P(both),
        P(None, both, "tp"),
        P(None, both, "tp"),
        P(None, both, "tp"),
        P(both, None),
        P(both, None),
    )
    out_specs = (
        P("fs", None, "tp"),
        P("fs", None, "tp"),
        P("fs", None, "tp"),
        P(both, "tp"),
    )
    return jax.shard_map(
        per_device, mesh=mesh, in_specs=in_specs, out_specs=out_specs, check_vma=False
    )
```
